32 devices in a mesh: grp: 2 (over y), sp: 4 (over z), tp: 4 (over x, core).
Axes of the slice: x: 2, y: 2, z: 4, core: 2. Of those that a mesh axis runs over, the one named last changes fastest.
Arguments:
- query_rows: bfloat16 [1024, 1024], P(('grp', 'sp'), 'tp'), parts along dimension 0, may hold values from -6 to 6
- key_rows: bfloat16 [1024, 1024], P(('grp', 'sp'), 'tp'), parts along dimension 0, may hold values from -6 to 6
- value_rows: bfloat16 [1024, 1024], P(('grp', 'sp'), 'tp'), parts along dimension 0, may hold values from -6 to 6
- gate_rows: bfloat16 [1024, 1024], P(('grp', 'sp'), 'tp'), parts along dimension 0, may hold values from -6 to 6
- log_decay: float32 [2, 8, 1024], P(None, 'tp', ('grp', 'sp')), parts along dimension 2, may hold values from -2 to 0, as said below
- head_gain: float32 [2, 1024], P(None, 'tp'), may hold values from 0.1 to 1.9
- out_weight: bfloat16 [1024, 2048], P('tp'), may hold values from -0.1875 to 0.1875
- residual: bfloat16 [1024, 2048], P(('grp', 'sp')), parts along dimension 0, may hold values from -6 to 6
- norm_gain: bfloat16 [2048], replicated, may hold values from 0.099609375 to 1.8984375
- gate_weight: bfloat16 [2048, 5632], P('sp', 'tp'), may hold values from -0.125 to 0.125
- up_weight: bfloat16 [2048, 5632], P('sp', 'tp'), may hold values from -0.125 to 0.125
- down_weight: bfloat16 [2048, 5632], P('sp', 'tp'), may hold values from -0.078125 to 0.078125
- gate_taps: bfloat16 [3, 5632], P(None, 'tp'), may hold values from -3.5 to 3.5
- up_taps: bfloat16 [3, 5632], P(None, 'tp'), may hold values from -3.5 to 3.5
Outputs:
- block_out: bfloat16 [1024, 2048], P(('grp', 'sp', 'tp')), parts along dimension 0
The draws below stay inside these ranges and needn't reach their ends.
There are 2 independent parts, one for each index of `grp`. The reference program is written for one: setup_inputs(seed, part) draws one part's arguments, and reference() takes and returns one part's arrays. A program takes and returns all parts, laid end to end along the dimension named above; an argument that names none is the same for every part. Nothing has to cross between parts.
Inputs may be any that keep to these rules, and one draw needn't show every extreme that they name: `log_decay`: every entry is negative.
All inputs are finite; a program needn't handle non-finite values.
Results may differ from the reference program's by a relative error of at most 0.017.
Values may be sent and summed in bfloat16 or wider, within the bound.
A program may use at most 64 MiB of HBM per device.

```python
import math
import jax
import jax.numpy as jnp
from jax import lax

D = 2048
RETENTION_HEADS = 8
HEAD = 128
FF = 5632
TOK_DEV = 128
VALUE = 1024
TOKENS = 512


def spread_log(subkey, shape, low_end, high_end):
    return jnp.exp(jax.random.uniform(subkey, shape, jnp.float32, jnp.log(low_end), jnp.log(high_end)))


def draw_log_decay(key, part):
    random_subkeys = jax.random.split(jax.random.fold_in(key, 17), 7)
    blocks = TOKENS // TOK_DEV
    slow_share = 0.5
    totals = spread_log(random_subkeys[1], (2, RETENTION_HEADS, 1), 0.2, 0.7)
    is_slow = jax.random.bernoulli(random_subkeys[0], slow_share, (2, RETENTION_HEADS, 1))
    reach_len = spread_log(random_subkeys[2], (2, RETENTION_HEADS, 1), 30.0, 100.0)
    baseline_decay_rate = jnp.where(is_slow, -totals / TOKENS, -1.0 / reach_len)
    multiplier = spread_log(random_subkeys[3], (2, RETENTION_HEADS, blocks, 1), 0.5, 1.5)
    multiplier = jnp.broadcast_to(multiplier, (2, RETENTION_HEADS, blocks, TOK_DEV)).reshape(2, RETENTION_HEADS, TOKENS)
    approximate_multiplier = jax.random.uniform(random_subkeys[4], (2, RETENTION_HEADS, TOKENS), jnp.float32, 0.6, 1.4)
    target_locations = jax.random.randint(random_subkeys[5], (2, RETENTION_HEADS, 2, 1), 0, TOKENS)
    spike_depth = jnp.log(jax.random.uniform(random_subkeys[6], (2, RETENTION_HEADS, 2, 1), jnp.float32, 0.55, 0.8))
    token_positions = jnp.arange(TOKENS)[None, None, None, :]
    spike_events = jnp.sum(jnp.where(token_positions == target_locations, spike_depth, 0.0), axis=2)
    return (baseline_decay_rate * multiplier * approximate_multiplier + spike_events).astype(jnp.float32)


def block_levels(key, shape, pieces, low, high):
    level, own = 1.0, jax.random.fold_in(key, 6)
    for position, blocks in pieces:
        draws = jnp.exp(jax.random.uniform(jax.random.fold_in(own, position), (blocks,), jnp.float32, low / len(pieces), high / len(pieces)))
        level = level * jnp.repeat(draws, shape[position] // blocks).reshape([-1 if axis == position else 1 for axis in range(len(shape))])
    return level


def normal_values(key, extent, scale, bound, cuts=(), dtype=jnp.bfloat16):
    entries = jax.random.normal(key, extent, jnp.float32) * scale
    if len(cuts) > 0:
        entries = block_levels(key, extent, cuts, -0.22, 0.18) * entries
    return jnp.clip(entries, min=-bound, max=bound).astype(dtype)


def setup_inputs(seed: int = 0, part: int = 0) -> dict:
    splits = jax.random.split(jax.random.key(seed), 15)
    part_keys = jax.random.split(jax.random.fold_in(splits[14], part), 15)
    query_rows = normal_values(part_keys[0], (TOKENS, VALUE), 1.0, 6.0, ((0, 4), (1, 4)))
    key_rows = normal_values(part_keys[1], (TOKENS, VALUE), 1.0, 6.0, ((0, 4), (1, 4)))
    value_rows = normal_values(part_keys[2], (TOKENS, VALUE), 1.0, 6.0, ((0, 4), (1, 4)))
    gate_rows = normal_values(part_keys[3], (TOKENS, VALUE), 1.0, 6.0, ((0, 4), (1, 4)))
    log_decay = draw_log_decay(jax.random.fold_in(jax.random.fold_in(splits[14], part), 71), part)
    head_gain = jnp.clip(1.0 + 0.18 * jax.random.normal(splits[5], (2, VALUE), jnp.float32), 0.1, 1.9)
    out_weight = normal_values(splits[6], (VALUE, D), VALUE ** -0.5, 0.1875, ((0, 4),))
    residual = normal_values(part_keys[7], (TOKENS, D), 1.0, 6.0, ((0, 4),))
    norm_gain = jnp.clip(1.0 + 0.18 * jax.random.normal(splits[8], (D,), jnp.float32), 0.099609375, 1.8984375).astype(jnp.bfloat16)
    gate_weight = normal_values(splits[9], (D, FF), D ** -0.5, 0.125, ((0, 4), (1, 4)))
    up_weight = normal_values(splits[10], (D, FF), D ** -0.5, 0.125, ((0, 4), (1, 4)))
    down_weight = normal_values(splits[11], (D, FF), FF ** -0.5, 0.078125, ((0, 4), (1, 4)))
    gate_taps = normal_values(splits[12], (3, FF), 3 ** -0.5, 3.5, ((1, 4),))
    up_taps = normal_values(splits[13], (3, FF), 3 ** -0.5, 3.5, ((1, 4),))
    return {"query_rows": query_rows, "key_rows": key_rows, "value_rows": value_rows, "gate_rows": gate_rows, "log_decay": log_decay, "head_gain": head_gain, "out_weight": out_weight, "residual": residual, "norm_gain": norm_gain, "gate_weight": gate_weight, "up_weight": up_weight, "down_weight": down_weight, "gate_taps": gate_taps, "up_taps": up_taps}


FULL_PRECISION = lax.Precision.HIGHEST
GROUP_EPS = 1e-05
NORM_EPS = 1e-06

def scan_retention(query_all, key_all, value_all, log_rates):
    length, head_count, head_width = query_all.shape
    block_len = math.gcd(length, 512)
    block_count = length // block_len
    query_blocks = query_all.reshape(block_count, block_len, head_count, head_width)
    key_blocks = key_all.reshape(block_count, block_len, head_count, head_width)
    value_blocks = value_all.reshape(block_count, block_len, head_count, head_width)
    rate_blocks = log_rates.T.reshape(block_count, block_len, head_count)
    lower_mask = jnp.arange(block_len)[:, None] >= jnp.arange(block_len)[None, :]

    def block_step(carry_state, inputs):
        query_blk, key_blk, value_blk, rate_blk = inputs
        cumul = jnp.cumsum(rate_blk, axis=0)
        gap_logs = cumul[:, None, :] - cumul[None, :, :]
        decay_mask = jnp.where(lower_mask[:, :, None], jnp.exp(jnp.minimum(gap_logs, 0.0)), 0.0)
        scores = jnp.einsum('thd,shd->tsh', query_blk, key_blk, precision=FULL_PRECISION) * decay_mask
        inner_part = jnp.einsum('tsh,she->the', scores, value_blk, precision=FULL_PRECISION)
        carried = jnp.einsum('thd,hde->the', query_blk * jnp.exp(cumul)[:, :, None], carry_state, precision=FULL_PRECISION)
        last_cumul = cumul[-1]
        key_decayed = key_blk * jnp.exp(last_cumul[None, :] - cumul)[:, :, None]
        new_state = carry_state * jnp.exp(last_cumul)[:, None, None] + jnp.einsum('shd,she->hde', key_decayed, value_blk, precision=FULL_PRECISION)
        return (new_state, inner_part + carried)
    zero_state = jnp.zeros((head_count, head_width, head_width), jnp.float32)
    ignored, block_outs = lax.scan(block_step, zero_state, (query_blocks, key_blocks, value_blocks, rate_blocks))
    return block_outs.reshape(length, head_count, head_width)

def group_norm(values):
    length, head_count, head_width = values.shape
    centre = values - lax.optimization_barrier(jnp.mean(values, axis=2, keepdims=True))
    spread = lax.optimization_barrier(jnp.mean(centre * centre, axis=2, keepdims=True))
    return (centre * lax.rsqrt(spread + GROUP_EPS)).reshape(length, head_count * head_width)

def rms_scale(middle, gain):
    values = middle.astype(jnp.float32)
    multiplier = lax.rsqrt(lax.optimization_barrier(jnp.mean(values * values, axis=1, keepdims=True)) + NORM_EPS)
    return (values * multiplier * gain.astype(jnp.float32)).astype(jnp.bfloat16)

def reference(query_rows, key_rows, value_rows, gate_rows, log_decay, head_gain, out_weight, residual, norm_gain, gate_weight, up_weight, down_weight, gate_taps, up_taps):
    key_scale = HEAD ** (-0.5)
    query_all = query_rows.astype(jnp.float32).reshape(TOKENS, RETENTION_HEADS, HEAD)
    key_all = key_rows.astype(jnp.float32).reshape(TOKENS, RETENTION_HEADS, HEAD) * key_scale
    value_all = value_rows.astype(jnp.float32).reshape(TOKENS, RETENTION_HEADS, HEAD)
    ahead_out = scan_retention(query_all, key_all, value_all, log_decay[0])
    behind_out = scan_retention(query_all[::-1], key_all[::-1], value_all[::-1], log_decay[1][:, ::-1])[::-1]
    combined = group_norm(ahead_out) * head_gain[0] + group_norm(behind_out) * head_gain[1]
    mixed_heads = (jax.nn.silu(gate_rows.astype(jnp.float32)) * combined).astype(jnp.bfloat16)
    attended = jnp.dot(mixed_heads, out_weight, preferred_element_type=jnp.float32)
    middle = lax.optimization_barrier((residual.astype(jnp.float32) + attended).astype(jnp.bfloat16))
    normed = rms_scale(middle, norm_gain)
    model_width = normed.shape[1]
    zero_row = jnp.zeros((1, model_width), jnp.bfloat16)
    padded = jnp.concatenate([zero_row, normed, zero_row], axis=0)
    block_len = math.gcd(TOKENS, 512)
    taps_gate = gate_taps.astype(jnp.float32)
    taps_up = up_taps.astype(jnp.float32)

    def one_block(block_index):
        first_row = (block_index * block_len).astype(jnp.int32)
        rows_with_rims = lax.dynamic_slice_in_dim(padded, first_row, block_len + 2, 0)
        pre_gate = lax.optimization_barrier(jnp.dot(rows_with_rims, gate_weight, preferred_element_type=jnp.float32).astype(jnp.bfloat16)).astype(jnp.float32)
        pre_up = lax.optimization_barrier(jnp.dot(rows_with_rims, up_weight, preferred_element_type=jnp.float32).astype(jnp.bfloat16)).astype(jnp.float32)
        conv_gate = taps_gate[0] * pre_gate[:-2] + taps_gate[1] * pre_gate[1:-1] + taps_gate[2] * pre_gate[2:]
        conv_up = taps_up[0] * pre_up[:-2] + taps_up[1] * pre_up[1:-1] + taps_up[2] * pre_up[2:]
        hidden = (jax.nn.silu(conv_gate) * conv_up).astype(jnp.bfloat16)
        ff_out = lax.dot_general(hidden, down_weight, (((1,), (1,)), ((), ())), preferred_element_type=jnp.float32)
        middle_rows = lax.dynamic_slice_in_dim(middle, first_row, block_len, 0).astype(jnp.float32)
        return (middle_rows + ff_out).astype(jnp.bfloat16)
    block_outs = lax.map(one_block, jnp.arange(TOKENS // block_len).astype(jnp.int32))
    return block_outs.reshape(TOKENS, model_width)
```

```python
import functools
import math

import jax
import jax.numpy as jnp
from jax import lax
from jax.experimental import pallas as pl
from jax.experimental.pallas import tpu as pltpu
from jax.sharding import PartitionSpec as P

HEAD = 128
PIECES = 2


FULL_PRECISION = lax.Precision.HIGHEST
GROUP_EPS = 1e-05
NORM_EPS = 1e-06


def prefix(value, axis, join, neutral, backward):
    count, mine = (lax.axis_size(axis), lax.axis_index(axis))
    pieces = jax.tree.map(lambda part: lax.all_gather(part, axis), value)
    if backward:
        pieces = jax.tree.map(lambda part: part[::-1], pieces)
        mine = count - 1 - mine
    running = jax.tree.map(
        lambda part, zero: jnp.full_like(part, 0) + jnp.asarray(zero, part.dtype), value, neutral
    )

    def lap(position, running):
        longer = join(running, jax.tree.map(lambda part: part[position], pieces))
        return jax.tree.map(lambda new, old: jnp.where(position < mine, new, old), longer, running)

    return lax.fori_loop(0, count - 1, lap, running)


def padded_2(shard, sides, width):
    for axis, dim in sides:
        size, length = (lax.axis_size(axis), shard.shape[dim])
        up = [(i, (i + 1) % size) for i in range(size - 1)]
        down = [(j, i) for i, j in up]
        last = lax.slice_in_dim(shard, length - width, length, axis=dim)
        initial = lax.slice_in_dim(shard, 0, width, axis=dim)
        before = lax.ppermute(last, axis, up)
        after = lax.ppermute(initial, axis, down)
        shard = jnp.concatenate([before, shard, after], axis=dim)
    return shard


def state_combine(earlier, later):
    return (earlier[0] * later[0], earlier[1] * later[0][:, None, None] + later[1])


def group_norm(values):
    length, head_count, head_width = values.shape
    centre = values - jnp.mean(values, axis=2, keepdims=True)
    spread = jnp.mean(centre * centre, axis=2, keepdims=True)
    return (centre * lax.rsqrt(spread + GROUP_EPS)).reshape(length, head_count * head_width)


def rms_scale(middle, gain):
    values = middle.astype(jnp.float32)
    multiplier = lax.rsqrt(jnp.mean(values * values, axis=1, keepdims=True) + NORM_EPS)
    return (values * multiplier * gain.astype(jnp.float32)).astype(jnp.bfloat16)


def local_retention(query_all, key_all, value_all, log_rates):
    length, head_count, head_width = query_all.shape
    block_len = math.gcd(length, 512)
    block_count = length // block_len
    cumul = jnp.cumsum(log_rates, axis=1).T
    query_block = query_all.reshape(block_count, block_len, head_count, head_width)
    key_block = key_all.reshape(block_count, block_len, head_count, head_width)
    value_block = value_all.reshape(block_count, block_len, head_count, head_width)
    cumul_block = cumul.reshape(block_count, block_len, head_count)
    before = jnp.concatenate(
        [jnp.zeros((1, head_count), jnp.float32), cumul_block[:-1, -1]], axis=0
    )
    local_cumul = cumul_block - before[:, None, :]
    gap_logs = local_cumul[:, :, None, :] - local_cumul[:, None, :, :]
    lower_mask = (jnp.arange(block_len)[:, None] >= jnp.arange(block_len)[None, :])[
        None, :, :, None
    ]
    decay_mask = jnp.where(lower_mask, jnp.exp(jnp.minimum(gap_logs, 0.0)), 0.0)
    scores = (
        jnp.einsum("bthd,bshd->btsh", query_block, key_block, precision=FULL_PRECISION) * decay_mask
    )
    inner_part = jnp.einsum("btsh,bshe->bthe", scores, value_block, precision=FULL_PRECISION)
    to_end = jnp.exp(local_cumul[:, -1:, :] - local_cumul)
    block_states = jnp.einsum(
        "bshd,bshe->bhde", key_block * to_end[..., None], value_block, precision=FULL_PRECISION
    )
    block_decay = jnp.exp(local_cumul[:, -1, :])

    def carry_step(carry_state, inputs):
        return (carry_state * inputs[0][:, None, None] + inputs[1], carry_state)

    zero_state = jnp.zeros((head_count, head_width, head_width), jnp.float32)
    end_state, entering = lax.scan(carry_step, zero_state, (block_decay, block_states))
    carried = jnp.einsum(
        "bthd,bhde->bthe",
        query_block * jnp.exp(local_cumul)[..., None],
        entering,
        precision=FULL_PRECISION,
    )
    output = (inner_part + carried).reshape(length, head_count, head_width)
    return (output, end_state, cumul, jnp.exp(cumul[-1]))


def with_incoming(output, query_all, cumul, incoming):
    return output + jnp.einsum(
        "thd,hde->the", query_all * jnp.exp(cumul)[:, :, None], incoming, precision=FULL_PRECISION
    )


def shards(
    query_rows,
    key_rows,
    value_rows,
    gate_rows,
    log_decay,
    head_gain,
    out_weight,
    residual,
    norm_gain,
    gate_weight,
    up_weight,
    down_weight,
    gate_taps,
    up_taps,
):
    pair_local = jnp.concatenate([gate_weight, up_weight], axis=1)
    row_count = query_rows.shape[0]
    head_count = query_rows.shape[1] // HEAD
    key_scale = HEAD ** (-0.5)
    query_all = query_rows.astype(jnp.float32).reshape(row_count, head_count, HEAD)
    key_all = key_rows.astype(jnp.float32).reshape(row_count, head_count, HEAD) * key_scale
    value_all = value_rows.astype(jnp.float32).reshape(row_count, head_count, HEAD)
    identity = (
        jnp.ones((head_count,), jnp.float32),
        jnp.zeros((head_count, HEAD, HEAD), jnp.float32),
    )
    ahead_local, ahead_state, ahead_cumul, ahead_decay = local_retention(
        query_all, key_all, value_all, log_decay[0]
    )
    query_back = query_all[::-1]
    behind_local, behind_state, behind_cumul, behind_decay = local_retention(
        query_back, key_all[::-1], value_all[::-1], log_decay[1][:, ::-1]
    )
    ahead_in = prefix((ahead_decay, ahead_state), "sp", state_combine, identity, False)[1]
    behind_in = prefix((behind_decay, behind_state), "sp", state_combine, identity, True)[1]
    ahead_out = with_incoming(ahead_local, query_all, ahead_cumul, ahead_in)
    behind_out = with_incoming(behind_local, query_back, behind_cumul, behind_in)[::-1]
    combined = group_norm(ahead_out) * head_gain[0] + group_norm(behind_out) * head_gain[1]
    mixed_heads = (jax.nn.silu(gate_rows.astype(jnp.float32)) * combined).astype(jnp.bfloat16)
    gathered = (
        lax.all_gather(pair_local, "sp", axis=0, tiled=True),
        lax.all_gather(down_weight, "sp", axis=0, tiled=True),
    )
    pair_full, down_full = gathered
    share_rows = row_count // lax.axis_size("tp")
    own_start = lax.axis_index("tp") * share_rows
    picked = mixed_heads
    attended = lax.psum_scatter(
        jnp.dot(picked, out_weight, preferred_element_type=jnp.float32).astype(jnp.bfloat16),
        "tp",
        scatter_dimension=0,
        tiled=True,
    ).astype(jnp.float32)
    residual_own = lax.dynamic_slice_in_dim(residual, own_start, share_rows, 0)
    middle_own = lax.optimization_barrier(
        (residual_own.astype(jnp.float32) + attended).astype(jnp.bfloat16)
    )
    normed = rms_scale(middle_own, norm_gain)
    pre_both = jnp.dot(
        lax.all_gather(normed, "tp", axis=0, tiled=True),
        pair_full,
        preferred_element_type=jnp.float32,
    ).astype(jnp.bfloat16)
    padded = padded_2(pre_both, (("sp", 0),), 1)
    half_width = gate_taps.shape[1]
    tap_table = jnp.concatenate([gate_taps, up_taps], axis=1).astype(jnp.float32)
    conv_out = (
        tap_table[0] * padded[:-2].astype(jnp.float32)
        + tap_table[1] * padded[1:-1].astype(jnp.float32)
        + tap_table[2] * padded[2:].astype(jnp.float32)
    )
    hidden = (jax.nn.silu(conv_out[:, :half_width]) * conv_out[:, half_width:]).astype(jnp.bfloat16)
    picked = hidden
    ff_out = lax.psum_scatter(
        lax.dot_general(
            picked, down_full, (((1,), (1,)), ((), ())), preferred_element_type=jnp.float32
        ).astype(jnp.bfloat16),
        "tp",
        scatter_dimension=0,
        tiled=True,
    ).astype(jnp.float32)
    return (middle_own.astype(jnp.float32) + ff_out).astype(jnp.bfloat16)


def block_kernel(
    spans,
    shares,
    pieces,
    query,
    key,
    value,
    gate,
    rates,
    gains,
    residual,
    norm_gain,
    gate_taps,
    up_taps,
    out_hbm,
    gate_hbm,
    up_hbm,
    down_hbm,
    result,
    keys,
    values,
    rate_all,
    out_w,
    pair_w,
    down_w,
    att_send,
    att_recv,
    middle_ref,
    norm_send,
    norm_all,
    part_send,
    part_own,
    part_recv,
    rim_send,
    rim_recv,
    hidden_all,
    tp_send,
    tp_recv,
    row_send,
    row_recv,
    local_sem,
    kv_sem,
    att_sem,
    norm_sem,
    fan_sem,
    part_sem,
    rim_sem,
    hid_sem,
    tp_sem,
    row_sem,
):
    me, lane = lax.axis_index("sp"), lax.axis_index("tp")
    rows, width = query.shape
    heads = width // HEAD
    share = rows // shares
    model = residual.shape[1]
    part_cols = model // spans
    f32, bf16 = jnp.float32, jnp.bfloat16
    sends = []

    def send(src, dst, sems, sp, tp):
        copy = pltpu.make_async_remote_copy(
            src_ref=src,
            dst_ref=dst,
            send_sem=sems.at[0],
            recv_sem=sems.at[1],
            device_id={"sp": sp, "tp": tp},
            device_id_type=pl.DeviceIdType.MESH,
        )
        copy.start()
        sends.append(copy)
        return copy

    def span_at(step):
        return lax.rem(me + step, spans)

    def share_at(step):
        return lax.rem(lane + step, shares)

    def span_rows(index):
        return pl.ds(pl.multiple_of(index * rows, rows), rows)

    loads = [
        pltpu.make_async_copy(src, dst, local_sem.at[i])
        for i, (src, dst) in enumerate(
            (
                (key, keys.at[span_rows(me)]),
                (value, values.at[span_rows(me)]),
                (rates, rate_all.at[me]),
                (out_hbm, out_w),
                (gate_hbm, pair_w.at[0]),
                (up_hbm, pair_w.at[1]),
                (down_hbm, down_w),
            )
        )
    ]
    for load in loads:
        load.start()
    barrier = pltpu.get_barrier_semaphore()
    for a in range(spans):
        for b in range(shares):
            if a or b:
                pl.semaphore_signal(
                    barrier,
                    inc=1,
                    device_id={"sp": span_at(a), "tp": share_at(b)},
                    device_id_type=pl.DeviceIdType.MESH,
                )
    pl.semaphore_wait(barrier, spans * shares - 1)

    arrivals = []
    for d in range(1, spans):
        to = span_at(d)
        arrivals += [
            send(rates, rate_all.at[me], kv_sem.at[d, 0], to, lane),
            send(key, keys.at[span_rows(me)], kv_sem.at[d, 1], to, lane),
            send(value, values.at[span_rows(me)], kv_sem.at[d, 2], to, lane),
        ]
    for load in loads[:3]:
        load.wait()
    for copy in arrivals:
        copy.wait_recv()

    low = lax.broadcasted_iota(jnp.int32, (rows, rows), 0)
    high = lax.broadcasted_iota(jnp.int32, (rows, rows), 1)
    upto = (low <= high).astype(f32)
    since = (low >= high).astype(f32)
    lines = rates.shape[0]
    offset = jnp.zeros((lines, 1), f32)
    offset_own = jnp.zeros((lines, 1), f32)
    cumuls = []
    for j in range(spans):
        offset_own = jnp.where(j == me, offset, offset_own)
        inside = jnp.dot(rate_all[j], upto, precision=FULL_PRECISION, preferred_element_type=f32)
        cumuls.append(inside + offset)
        offset = offset + inside[:, rows - 1 :]
    cumul = jnp.concatenate(cumuls, axis=1)
    every_rate = jnp.concatenate([rate_all[j] for j in range(spans)], axis=1)
    own_rate = rates[...]
    own_cumul = lax.dot_general(
        since,
        own_rate,
        (((1,), (1,)), ((), ())),
        precision=FULL_PRECISION,
        preferred_element_type=f32,
    )
    own_before = lax.dot_general(
        (low > high).astype(f32),
        own_rate,
        (((1,), (1,)), ((), ())),
        precision=FULL_PRECISION,
        preferred_element_type=f32,
    )
    total = spans * rows
    mine_at = lax.broadcasted_iota(jnp.int32, (rows, total), 0) + me * rows
    other_at = lax.broadcasted_iota(jnp.int32, (rows, total), 1)
    mixed = []
    for head in range(heads):
        cols = slice(head * HEAD, (head + 1) * HEAD)
        scores = lax.dot_general(
            query[:, cols],
            keys[:, cols],
            (((1,), (1,)), ((), ())),
            preferred_element_type=f32,
        ) * (HEAD ** (-0.5))
        back = heads + head
        ahead_gap = (own_cumul[:, head : head + 1] + offset_own[head : head + 1]) - cumul[
            head : head + 1
        ]
        behind_gap = (cumul[back : back + 1] - every_rate[back : back + 1]) - (
            own_before[:, back : back + 1] + offset_own[back : back + 1]
        )
        sides = []
        for gap, keep, row in (
            (ahead_gap, mine_at >= other_at, 0),
            (behind_gap, mine_at <= other_at, 1),
        ):
            weighted = jnp.where(keep, jnp.exp(jnp.minimum(gap, 0.0)), 0.0) * scores
            top = weighted.astype(bf16)
            rest = (weighted - top.astype(f32)).astype(bf16)
            held = values[:, cols]
            out = jnp.dot(top, held, preferred_element_type=f32) + jnp.dot(
                rest, held, preferred_element_type=f32
            )
            centre = out - jnp.mean(out, axis=1, keepdims=True)
            spread = jnp.mean(centre * centre, axis=1, keepdims=True)
            sides.append(centre * lax.rsqrt(spread + GROUP_EPS) * gains[row : row + 1, cols])
        level = gate[:, cols].astype(f32)
        mixed.append(((level / (1.0 + jnp.exp(-level))) * (sides[0] + sides[1])).astype(bf16))
    mixed = jnp.concatenate(mixed, axis=1)

    loads[3].wait()
    step_cols = math.gcd(model, 512)
    for at in range(0, model, step_cols):
        att_send[:, at : at + step_cols] = jnp.dot(
            mixed, out_w[:, at : at + step_cols], preferred_element_type=f32
        ).astype(bf16)

    def share_rows(index):
        return pl.ds(pl.multiple_of(index * share, share), share)

    arrivals = [
        send(
            att_send.at[share_rows(share_at(d))],
            att_recv.at[d],
            att_sem.at[d],
            me,
            share_at(d),
        )
        for d in range(1, shares)
    ]
    attended = att_send[share_rows(lane), :].astype(f32)
    for d, copy in enumerate(arrivals, 1):
        copy.wait_recv()
        attended = attended + att_recv[d].astype(f32)
    middle = (residual[share_rows(lane), :].astype(f32) + attended).astype(bf16)
    middle_ref[...] = middle
    middle = middle.astype(f32)
    factor = lax.rsqrt(jnp.mean(middle * middle, axis=1, keepdims=True) + NORM_EPS)
    normed = (middle * factor * norm_gain[...].astype(f32)).astype(bf16)
    for j in range(spans):
        norm_send[j] = normed[:, j * part_cols : (j + 1) * part_cols]

    def token_rows(span, tp):
        return pl.ds(pl.multiple_of(span * rows + tp * share, share), share)

    arrivals = [
        send(
            norm_send.at[span_at(d)],
            norm_all.at[token_rows(me, lane)],
            norm_sem.at[d],
            span_at(d),
            lane,
        )
        for d in range(1, spans)
    ]
    norm_all[token_rows(me, lane), :] = norm_send[me]
    fans = {}
    for d in (0, *range(1, spans)):
        source = lax.rem(me + spans - d, spans)
        if d:
            arrivals[d - 1].wait_recv()
        block = norm_send.at[me] if d == 0 else norm_all.at[token_rows(source, lane)]
        for b in range(1, shares):
            fans[d, b] = send(
                block, norm_all.at[token_rows(source, lane)], fan_sem.at[d, b], me, share_at(b)
            )
    for copy in fans.values():
        copy.wait_recv()

    loads[4].wait()
    loads[5].wait()
    far_first = sorted(range(1, spans), key=lambda d: -min(d, spans - d))
    parts = {}
    for c, (start, size) in enumerate(pieces):
        cols = slice(start, start + size)
        for d in far_first + [0]:
            block = norm_all[span_rows(span_at(d)), :]
            for g in range(2):
                product = jnp.dot(block, pair_w[g, :, cols], preferred_element_type=f32)
                if d == 0:
                    part_own[g, :, cols] = product
                else:
                    part_send[d, g, :, cols] = product.astype(bf16)
            if d:
                for g in range(2):
                    parts[c, d, g] = send(
                        part_send.at[d, g, :, pl.ds(start, size)],
                        part_recv.at[d, g, :, pl.ds(start, size)],
                        part_sem.at[c, d, g],
                        span_at(d),
                        lane,
                    )

    row_at = lax.broadcasted_iota(jnp.int32, (rows, 1), 0)
    hidden_copies = {}
    for c, (start, size) in enumerate(pieces):
        cols = slice(start, start + size)
        for d in range(1, spans):
            for g in range(2):
                parts[c, d, g].wait_recv()
        for g in range(2):
            summed = part_own[g, :, cols]
            for d in range(1, spans):
                summed = summed + part_recv[d, g, :, cols].astype(f32)
            summed = summed.astype(bf16).astype(f32)
            part_own[g, :, cols] = summed
            rim_send[c, 0, g : g + 1, :size] = summed[rows - 1 :]
            rim_send[c, 1, g : g + 1, :size] = summed[:1]
        rims = [
            send(
                rim_send.at[c, way, :, pl.ds(0, size)],
                rim_recv.at[c, way, :, pl.ds(0, size)],
                rim_sem.at[c, way],
                span_at(1 if way == 0 else spans - 1),
                lane,
            )
            for way in range(2)
        ]
        for rim in rims:
            rim.wait_recv()
        convs = []
        for g, taps in enumerate((gate_taps, up_taps)):
            here = part_own[g, :, cols]
            above = jnp.where(me > 0, rim_recv[c, 0, g : g + 1, :size], 0.0)
            below = jnp.where(me < spans - 1, rim_recv[c, 1, g : g + 1, :size], 0.0)
            earlier = jnp.where(row_at == 0, above, pltpu.roll(here, 1, 0))
            later = jnp.where(row_at == rows - 1, below, pltpu.roll(here, rows - 1, 0))
            weight = taps[:, cols].astype(f32)
            convs.append(weight[0:1] * earlier + weight[1:2] * here + weight[2:3] * later)
        hidden_all[span_rows(me), cols] = (
            (convs[0] / (1.0 + jnp.exp(-convs[0]))) * convs[1]
        ).astype(bf16)
        for d in far_first:
            block = hidden_all.at[span_rows(me), pl.ds(start, size)]
            hidden_copies[c, d] = send(block, block, hid_sem.at[c, d], span_at(d), lane)

    loads[6].wait()
    near_first = [0] + far_first[::-1]
    fans = {}
    for d in near_first:
        source = lax.rem(me + spans - d, spans)
        if d:
            for c in range(len(pieces)):
                hidden_copies[c, d].wait_recv()
        tp_send[d] = lax.dot_general(
            hidden_all[span_rows(source), :],
            down_w[...],
            (((1,), (1,)), ((), ())),
            preferred_element_type=f32,
        ).astype(bf16)
        for b in range(1, shares):
            fans[d, b] = send(
                tp_send.at[d, share_rows(share_at(b))],
                tp_recv.at[d, b],
                tp_sem.at[d, b],
                me,
                share_at(b),
            )
    arrivals = []
    for d in near_first:
        source = lax.rem(me + spans - d, spans)
        summed = tp_send[d, share_rows(lane), :].astype(f32)
        for b in range(1, shares):
            fans[d, b].wait_recv()
            summed = summed + tp_recv[d, b].astype(f32)
        row_send[d] = summed.astype(bf16)
        if d:
            arrivals.append(send(row_send.at[d], row_recv.at[me], row_sem.at[d], source, lane))
        else:
            row_recv[me] = row_send[0]
    for copy in arrivals:
        copy.wait_recv()
    for j in range(spans):
        cols = slice(j * part_cols, (j + 1) * part_cols)
        result[:, cols] = (middle_ref[:, cols].astype(f32) + row_recv[j].astype(f32)).astype(bf16)
    for copy in sends:
        copy.wait_send()


def fused_block(
    query_rows,
    key_rows,
    value_rows,
    gate_rows,
    log_decay,
    head_gain,
    out_weight,
    residual,
    norm_gain,
    gate_weight,
    up_weight,
    down_weight,
    gate_taps,
    up_taps,
):
    spans, shares = (lax.axis_size("sp"), lax.axis_size("tp"))
    rows, width = query_rows.shape
    model = residual.shape[1]
    units = gate_weight.shape[1]
    part_cols, share = (model // spans, rows // shares)
    total = spans * rows
    lanes = units // 128
    count = min(PIECES, lanes)
    pieces, at = [], 0
    for c in range(count):
        size = (lanes // count + (c < lanes % count)) * 128
        pieces.append((at, size))
        at += size
    widest = pieces[0][1]
    lines = log_decay.shape[0] * log_decay.shape[1]
    rates = log_decay.reshape(lines, rows)
    f32, bf16 = jnp.float32, jnp.bfloat16
    vmem = pl.BlockSpec(memory_space=pltpu.VMEM)
    far = pl.BlockSpec(memory_space=pl.ANY)
    dma = pltpu.SemaphoreType.DMA
    return pl.pallas_call(
        functools.partial(block_kernel, spans, shares, tuple(pieces)),
        out_shape=jax.ShapeDtypeStruct((share, model), bf16),
        in_specs=[vmem] * 10 + [far] * 4,
        out_specs=vmem,
        scratch_shapes=[
            pltpu.VMEM((total, width), bf16),
            pltpu.VMEM((total, width), bf16),
            pltpu.VMEM((spans, lines, rows), f32),
            pltpu.VMEM(out_weight.shape, bf16),
            pltpu.VMEM((2, *gate_weight.shape), bf16),
            pltpu.VMEM(down_weight.shape, bf16),
            pltpu.VMEM((rows, model), bf16),
            pltpu.VMEM((shares, share, model), bf16),
            pltpu.VMEM((share, model), bf16),
            pltpu.VMEM((spans, share, part_cols), bf16),
            pltpu.VMEM((total, part_cols), bf16),
            pltpu.VMEM((spans, 2, rows, units), bf16),
            pltpu.VMEM((2, rows, units), f32),
            pltpu.VMEM((spans, 2, rows, units), bf16),
            pltpu.VMEM((count, 2, 2, widest), f32),
            pltpu.VMEM((count, 2, 2, widest), f32),
            pltpu.VMEM((total, units), bf16),
            pltpu.VMEM((spans, rows, part_cols), bf16),
            pltpu.VMEM((spans, shares, share, part_cols), bf16),
            pltpu.VMEM((spans, share, part_cols), bf16),
            pltpu.VMEM((spans, share, part_cols), bf16),
            dma((7,)),
            dma((spans, 3, 2)),
            dma((shares, 2)),
            dma((spans, 2)),
            dma((spans, shares, 2)),
            dma((count, spans, 2, 2)),
            dma((count, 2, 2)),
            dma((count, spans, 2)),
            dma((spans, shares, 2)),
            dma((spans, 2)),
        ],
        compiler_params=pltpu.CompilerParams(collective_id=0, has_side_effects=True),
    )(
        query_rows,
        key_rows,
        value_rows,
        gate_rows,
        rates,
        head_gain,
        residual,
        norm_gain.reshape(1, model),
        gate_taps,
        up_taps,
        out_weight,
        gate_weight,
        up_weight,
        down_weight,
    )


def either(*args):
    span_tokens = args[0].shape[0] * lax.axis_size("sp")
    model_width = args[7].shape[1]
    if span_tokens < model_width:
        return fused_block(*args)
    return shards(*args)


def solution(mesh):
    in_specs = (
        P(("grp", "sp"), "tp"),
        P(("grp", "sp"), "tp"),
        P(("grp", "sp"), "tp"),
        P(("grp", "sp"), "tp"),
        P(None, "tp", ("grp", "sp")),
        P(None, "tp"),
        P("tp", None),
        P(("grp", "sp"), None),
        P(),
        P("sp", "tp"),
        P("sp", "tp"),
        P("sp", "tp"),
        P(None, "tp"),
        P(None, "tp"),
    )
    out_specs = P(("grp", "sp", "tp"), None)
    return jax.shard_map(either, mesh=mesh, in_specs=in_specs, out_specs=out_specs, check_vma=False)
```

```python
import functools
import math

import jax
import jax.numpy as jnp
from jax import lax
from jax.experimental import pallas as pl
from jax.experimental.pallas import tpu as pltpu
from jax.sharding import PartitionSpec as P

HEAD = 128
PIECES = 12
EDGE = 16
FLIGHT = 2
HEADSTART = 2
SKEW = 2


FULL_PRECISION = lax.Precision.HIGHEST
GROUP_EPS = 1e-05
NORM_EPS = 1e-06


def prefix(value, axis, join, neutral, backward):
    count, mine = (lax.axis_size(axis), lax.axis_index(axis))
    pieces = jax.tree.map(lambda part: lax.all_gather(part, axis), value)
    if backward:
        pieces = jax.tree.map(lambda part: part[::-1], pieces)
        mine = count - 1 - mine
    running = jax.tree.map(
        lambda part, zero: jnp.full_like(part, 0) + jnp.asarray(zero, part.dtype), value, neutral
    )

    def lap(position, running):
        longer = join(running, jax.tree.map(lambda part: part[position], pieces))
        return jax.tree.map(lambda new, old: jnp.where(position < mine, new, old), longer, running)

    return lax.fori_loop(0, count - 1, lap, running)


def padded_2(shard, sides, width):
    for axis, dim in sides:
        size, length = (lax.axis_size(axis), shard.shape[dim])
        up = [(i, (i + 1) % size) for i in range(size - 1)]
        down = [(j, i) for i, j in up]
        last = lax.slice_in_dim(shard, length - width, length, axis=dim)
        initial = lax.slice_in_dim(shard, 0, width, axis=dim)
        before = lax.ppermute(last, axis, up)
        after = lax.ppermute(initial, axis, down)
        shard = jnp.concatenate([before, shard, after], axis=dim)
    return shard


def state_combine(earlier, later):
    return (earlier[0] * later[0], earlier[1] * later[0][:, None, None] + later[1])


def group_norm(values):
    length, head_count, head_width = values.shape
    centre = values - jnp.mean(values, axis=2, keepdims=True)
    spread = jnp.mean(centre * centre, axis=2, keepdims=True)
    return (centre * lax.rsqrt(spread + GROUP_EPS)).reshape(length, head_count * head_width)


def rms_scale(middle, gain):
    values = middle.astype(jnp.float32)
    multiplier = lax.rsqrt(jnp.mean(values * values, axis=1, keepdims=True) + NORM_EPS)
    return (values * multiplier * gain.astype(jnp.float32)).astype(jnp.bfloat16)


def local_retention(query_all, key_all, value_all, log_rates):
    length, head_count, head_width = query_all.shape
    block_len = math.gcd(length, 512)
    block_count = length // block_len
    cumul = jnp.cumsum(log_rates, axis=1).T
    query_block = query_all.reshape(block_count, block_len, head_count, head_width)
    key_block = key_all.reshape(block_count, block_len, head_count, head_width)
    value_block = value_all.reshape(block_count, block_len, head_count, head_width)
    cumul_block = cumul.reshape(block_count, block_len, head_count)
    before = jnp.concatenate(
        [jnp.zeros((1, head_count), jnp.float32), cumul_block[:-1, -1]], axis=0
    )
    local_cumul = cumul_block - before[:, None, :]
    gap_logs = local_cumul[:, :, None, :] - local_cumul[:, None, :, :]
    lower_mask = (jnp.arange(block_len)[:, None] >= jnp.arange(block_len)[None, :])[
        None, :, :, None
    ]
    decay_mask = jnp.where(lower_mask, jnp.exp(jnp.minimum(gap_logs, 0.0)), 0.0)
    scores = (
        jnp.einsum("bthd,bshd->btsh", query_block, key_block, precision=FULL_PRECISION) * decay_mask
    )
    inner_part = jnp.einsum("btsh,bshe->bthe", scores, value_block, precision=FULL_PRECISION)
    to_end = jnp.exp(local_cumul[:, -1:, :] - local_cumul)
    block_states = jnp.einsum(
        "bshd,bshe->bhde", key_block * to_end[..., None], value_block, precision=FULL_PRECISION
    )
    block_decay = jnp.exp(local_cumul[:, -1, :])

    def carry_step(carry_state, inputs):
        return (carry_state * inputs[0][:, None, None] + inputs[1], carry_state)

    zero_state = jnp.zeros((head_count, head_width, head_width), jnp.float32)
    end_state, entering = lax.scan(carry_step, zero_state, (block_decay, block_states))
    carried = jnp.einsum(
        "bthd,bhde->bthe",
        query_block * jnp.exp(local_cumul)[..., None],
        entering,
        precision=FULL_PRECISION,
    )
    output = (inner_part + carried).reshape(length, head_count, head_width)
    return (output, end_state, cumul, jnp.exp(cumul[-1]))


def with_incoming(output, query_all, cumul, incoming):
    return output + jnp.einsum(
        "thd,hde->the", query_all * jnp.exp(cumul)[:, :, None], incoming, precision=FULL_PRECISION
    )


def shards(
    query_rows,
    key_rows,
    value_rows,
    gate_rows,
    log_decay,
    head_gain,
    out_weight,
    residual,
    norm_gain,
    gate_weight,
    up_weight,
    down_weight,
    gate_taps,
    up_taps,
):
    pair_local = jnp.concatenate([gate_weight, up_weight], axis=1)
    row_count = query_rows.shape[0]
    head_count = query_rows.shape[1] // HEAD
    key_scale = HEAD ** (-0.5)
    query_all = query_rows.astype(jnp.float32).reshape(row_count, head_count, HEAD)
    key_all = key_rows.astype(jnp.float32).reshape(row_count, head_count, HEAD) * key_scale
    value_all = value_rows.astype(jnp.float32).reshape(row_count, head_count, HEAD)
    identity = (
        jnp.ones((head_count,), jnp.float32),
        jnp.zeros((head_count, HEAD, HEAD), jnp.float32),
    )
    ahead_local, ahead_state, ahead_cumul, ahead_decay = local_retention(
        query_all, key_all, value_all, log_decay[0]
    )
    query_back = query_all[::-1]
    behind_local, behind_state, behind_cumul, behind_decay = local_retention(
        query_back, key_all[::-1], value_all[::-1], log_decay[1][:, ::-1]
    )
    ahead_in = prefix((ahead_decay, ahead_state), "sp", state_combine, identity, False)[1]
    behind_in = prefix((behind_decay, behind_state), "sp", state_combine, identity, True)[1]
    ahead_out = with_incoming(ahead_local, query_all, ahead_cumul, ahead_in)
    behind_out = with_incoming(behind_local, query_back, behind_cumul, behind_in)[::-1]
    combined = group_norm(ahead_out) * head_gain[0] + group_norm(behind_out) * head_gain[1]
    mixed_heads = (jax.nn.silu(gate_rows.astype(jnp.float32)) * combined).astype(jnp.bfloat16)
    gathered = (
        lax.all_gather(pair_local, "sp", axis=0, tiled=True),
        lax.all_gather(down_weight, "sp", axis=0, tiled=True),
    )
    pair_full, down_full = gathered
    share_rows = row_count // lax.axis_size("tp")
    own_start = lax.axis_index("tp") * share_rows
    picked = mixed_heads
    attended = lax.psum_scatter(
        jnp.dot(picked, out_weight, preferred_element_type=jnp.float32).astype(jnp.bfloat16),
        "tp",
        scatter_dimension=0,
        tiled=True,
    ).astype(jnp.float32)
    residual_own = lax.dynamic_slice_in_dim(residual, own_start, share_rows, 0)
    middle_own = lax.optimization_barrier(
        (residual_own.astype(jnp.float32) + attended).astype(jnp.bfloat16)
    )
    normed = rms_scale(middle_own, norm_gain)
    pre_both = jnp.dot(
        lax.all_gather(normed, "tp", axis=0, tiled=True),
        pair_full,
        preferred_element_type=jnp.float32,
    ).astype(jnp.bfloat16)
    padded = padded_2(pre_both, (("sp", 0),), 1)
    half_width = gate_taps.shape[1]
    tap_table = jnp.concatenate([gate_taps, up_taps], axis=1).astype(jnp.float32)
    conv_out = (
        tap_table[0] * padded[:-2].astype(jnp.float32)
        + tap_table[1] * padded[1:-1].astype(jnp.float32)
        + tap_table[2] * padded[2:].astype(jnp.float32)
    )
    hidden = (jax.nn.silu(conv_out[:, :half_width]) * conv_out[:, half_width:]).astype(jnp.bfloat16)
    picked = hidden
    ff_out = lax.psum_scatter(
        lax.dot_general(
            picked, down_full, (((1,), (1,)), ((), ())), preferred_element_type=jnp.float32
        ).astype(jnp.bfloat16),
        "tp",
        scatter_dimension=0,
        tiled=True,
    ).astype(jnp.float32)
    return (middle_own.astype(jnp.float32) + ff_out).astype(jnp.bfloat16)


def block_kernel(
    spans,
    shares,
    pieces,
    query,
    key,
    value,
    gate,
    rates,
    gains,
    residual,
    norm_gain,
    gate_taps,
    up_taps,
    out_hbm,
    gate_hbm,
    up_hbm,
    down_hbm,
    result,
    keys,
    values,
    rate_all,
    out_w,
    pair_w,
    down_w,
    att_send,
    att_recv,
    middle_ref,
    norm_send,
    norm_all,
    part_send,
    part_own,
    part_recv,
    hidden_all,
    tp_send,
    tp_recv,
    row_send,
    row_recv,
    local_sem,
    kv_sem,
    att_sem,
    norm_sem,
    fan_sem,
    part_sem,
    hid_sem,
    tp_sem,
    row_sem,
):
    me, lane = lax.axis_index("sp"), lax.axis_index("tp")
    rows, width = query.shape
    heads = width // HEAD
    share = rows // shares
    model = residual.shape[1]
    part_cols = model // spans
    f32, bf16 = jnp.float32, jnp.bfloat16
    sends = []

    def send(src, dst, sems, sp, tp):
        copy = pltpu.make_async_remote_copy(
            src_ref=src,
            dst_ref=dst,
            send_sem=sems.at[0],
            recv_sem=sems.at[1],
            device_id={"sp": sp, "tp": tp},
            device_id_type=pl.DeviceIdType.MESH,
        )
        copy.start()
        sends.append(copy)
        return copy

    def span_at(step):
        return lax.rem(me + step, spans)

    def share_at(step):
        return lax.rem(lane + step, shares)

    def span_rows(index):
        return pl.ds(pl.multiple_of(index * rows, rows), rows)

    loads = [
        pltpu.make_async_copy(src, dst, local_sem.at[i])
        for i, (src, dst) in enumerate(
            (
                (key, keys.at[span_rows(me)]),
                (value, values.at[span_rows(me)]),
                (rates, rate_all.at[me]),
                (out_hbm, out_w),
                (gate_hbm, pair_w.at[0]),
                (up_hbm, pair_w.at[1]),
                (down_hbm, down_w),
            )
        )
    ]
    for load in loads:
        load.start()
    barrier = pltpu.get_barrier_semaphore()
    for a in range(spans):
        for b in range(shares):
            if a or b:
                pl.semaphore_signal(
                    barrier,
                    inc=1,
                    device_id={"sp": span_at(a), "tp": share_at(b)},
                    device_id_type=pl.DeviceIdType.MESH,
                )
    pl.semaphore_wait(barrier, spans * shares - 1)

    arrivals = []
    for d in range(1, spans):
        to = span_at(d)
        arrivals += [
            send(rates, rate_all.at[me], kv_sem.at[d, 0], to, lane),
            send(key, keys.at[span_rows(me)], kv_sem.at[d, 1], to, lane),
            send(value, values.at[span_rows(me)], kv_sem.at[d, 2], to, lane),
        ]
    for load in loads[:3]:
        load.wait()
    for copy in arrivals:
        copy.wait_recv()

    low = lax.broadcasted_iota(jnp.int32, (rows, rows), 0)
    high = lax.broadcasted_iota(jnp.int32, (rows, rows), 1)
    upto = (low <= high).astype(f32)
    since = (low >= high).astype(f32)
    lines = rates.shape[0]
    offset = jnp.zeros((lines, 1), f32)
    offset_own = jnp.zeros((lines, 1), f32)
    cumuls = []
    for j in range(spans):
        offset_own = jnp.where(j == me, offset, offset_own)
        inside = jnp.dot(rate_all[j], upto, precision=FULL_PRECISION, preferred_element_type=f32)
        cumuls.append(inside + offset)
        offset = offset + inside[:, rows - 1 :]
    cumul = jnp.concatenate(cumuls, axis=1)
    every_rate = jnp.concatenate([rate_all[j] for j in range(spans)], axis=1)
    own_rate = rates[...]
    own_cumul = lax.dot_general(
        since,
        own_rate,
        (((1,), (1,)), ((), ())),
        precision=FULL_PRECISION,
        preferred_element_type=f32,
    )
    own_before = lax.dot_general(
        (low > high).astype(f32),
        own_rate,
        (((1,), (1,)), ((), ())),
        precision=FULL_PRECISION,
        preferred_element_type=f32,
    )
    total = spans * rows
    mine_at = lax.broadcasted_iota(jnp.int32, (rows, total), 0) + me * rows
    other_at = lax.broadcasted_iota(jnp.int32, (rows, total), 1)
    mixed = []
    for head in range(heads):
        cols = slice(head * HEAD, (head + 1) * HEAD)
        scores = lax.dot_general(
            query[:, cols],
            keys[:, cols],
            (((1,), (1,)), ((), ())),
            preferred_element_type=f32,
        ) * (HEAD ** (-0.5))
        back = heads + head
        ahead_gap = (own_cumul[:, head : head + 1] + offset_own[head : head + 1]) - cumul[
            head : head + 1
        ]
        behind_gap = (cumul[back : back + 1] - every_rate[back : back + 1]) - (
            own_before[:, back : back + 1] + offset_own[back : back + 1]
        )
        sides = []
        for gap, keep, row in (
            (ahead_gap, mine_at >= other_at, 0),
            (behind_gap, mine_at <= other_at, 1),
        ):
            weighted = jnp.where(keep, jnp.exp(jnp.minimum(gap, 0.0)), 0.0) * scores
            top = weighted.astype(bf16)
            rest = (weighted - top.astype(f32)).astype(bf16)
            held = values[:, cols]
            out = jnp.dot(top, held, preferred_element_type=f32) + jnp.dot(
                rest, held, preferred_element_type=f32
            )
            centre = out - jnp.mean(out, axis=1, keepdims=True)
            spread = jnp.mean(centre * centre, axis=1, keepdims=True)
            sides.append(centre * lax.rsqrt(spread + GROUP_EPS) * gains[row : row + 1, cols])
        level = gate[:, cols].astype(f32)
        mixed.append(((level / (1.0 + jnp.exp(-level))) * (sides[0] + sides[1])).astype(bf16))
    mixed = jnp.concatenate(mixed, axis=1)

    loads[3].wait()
    step_cols = math.gcd(model, 512)
    for at in range(0, model, step_cols):
        att_send[:, at : at + step_cols] = jnp.dot(
            mixed, out_w[:, at : at + step_cols], preferred_element_type=f32
        ).astype(bf16)

    def share_rows(index):
        return pl.ds(pl.multiple_of(index * share, share), share)

    arrivals = [
        send(
            att_send.at[share_rows(share_at(d))],
            att_recv.at[d],
            att_sem.at[d],
            me,
            share_at(d),
        )
        for d in range(1, shares)
    ]
    attended = att_send[share_rows(lane), :].astype(f32)
    for d, copy in enumerate(arrivals, 1):
        copy.wait_recv()
        attended = attended + att_recv[d].astype(f32)
    middle = (residual[share_rows(lane), :].astype(f32) + attended).astype(bf16)
    middle_ref[...] = middle
    middle = middle.astype(f32)
    factor = lax.rsqrt(jnp.mean(middle * middle, axis=1, keepdims=True) + NORM_EPS)
    normed = (middle * factor * norm_gain[...].astype(f32)).astype(bf16)
    for j in range(spans):
        norm_send[j] = normed[:, j * part_cols : (j + 1) * part_cols]

    def token_rows(span, tp):
        return pl.ds(pl.multiple_of(span * rows + tp * share, share), share)

    arrivals = [
        send(
            norm_send.at[span_at(d)],
            norm_all.at[token_rows(me, lane)],
            norm_sem.at[d],
            span_at(d),
            lane,
        )
        for d in range(1, spans)
    ]
    norm_all[token_rows(me, lane), :] = norm_send[me]
    fans = {}
    for d in (0, *range(1, spans)):
        source = lax.rem(me + spans - d, spans)
        if d:
            arrivals[d - 1].wait_recv()
        block = norm_send.at[me] if d == 0 else norm_all.at[token_rows(source, lane)]
        for b in range(1, shares):
            fans[d, b] = send(
                block, norm_all.at[token_rows(source, lane)], fan_sem.at[d, b], me, share_at(b)
            )
    for copy in fans.values():
        copy.wait_recv()

    loads[4].wait()
    loads[5].wait()
    last = spans - 1
    half = spans * rows // 2
    reach = half + EDGE
    size = pieces[0][1]
    origins, owners = (last, 0), (0, last)

    def part_copy(way, c):
        return pltpu.make_async_remote_copy(
            src_ref=part_send.at[way, c],
            dst_ref=part_recv.at[way, c],
            send_sem=part_sem.at[way, c, 0],
            recv_sem=part_sem.at[way, c, 1],
            device_id={"sp": span_at(spans - 1 if way == 0 else 1), "tp": lane},
            device_id_type=pl.DeviceIdType.MESH,
        )

    def hidden_copy(way, c):
        block = hidden_all.at[pl.ds(way * half, half), pl.ds(pieces[c][0], size)]
        return pltpu.make_async_remote_copy(
            src_ref=block,
            dst_ref=block,
            send_sem=hid_sem.at[way, c, 0],
            recv_sem=hid_sem.at[way, c, 1],
            device_id={"sp": span_at(1 if way == 0 else spans - 1), "tp": lane},
            device_id_type=pl.DeviceIdType.MESH,
        )

    def start_part(way, c):
        @pl.when(me == origins[way])
        def _():
            if c >= FLIGHT:
                part_copy(way, c - FLIGHT).wait_send()
            part_copy(way, c).start()

    def start_hidden(way, c):
        @pl.when(me == owners[way])
        def _():
            if c >= FLIGHT:
                hidden_copy(way, c - FLIGHT).wait_send()
            hidden_copy(way, c).start()

    for c, (start, _) in enumerate(pieces):
        cols = slice(start, start + size)
        for way in range(2):
            at = way * (half - EDGE)
            block = norm_all[at : at + reach, :]
            products = [
                jnp.dot(block, pair_w[g, :, cols], preferred_element_type=f32) for g in range(2)
            ]

            @pl.when(me == origins[way])
            def _():
                for g in range(2):
                    part_send[way, c, g] = products[g].astype(bf16)

            if c < HEADSTART:
                start_part(way, c)

            @pl.when(me != origins[way])
            def _():
                for g in range(2):
                    part_own[way, c, g] = products[g]

    row_at = lax.broadcasted_iota(jnp.int32, (reach, 1), 0)
    issued = 0
    hops = (last - me, me)
    for turn in range(len(pieces) + SKEW * (last - 1)):
        if turn + HEADSTART < len(pieces):
            for way in range(2):
                start_part(way, turn + HEADSTART)
        for way in range(2):
            for hop in range(1, last):
                c = turn - SKEW * (hop - 1)
                if 0 <= c < len(pieces):

                    @pl.when(hops[way] == hop)
                    def _():
                        part_copy(way, c).wait_recv()
                        for g in range(2):
                            part_send[way, c, g] = (
                                part_own[way, c, g] + part_recv[way, c, g].astype(f32)
                            ).astype(bf16)
                        part_copy(way, c).start()

            c = turn - SKEW * (last - 1)
            if c < 0:
                continue
            cols = slice(pieces[c][0], pieces[c][0] + size)

            @pl.when(me == owners[way])
            def _():
                part_copy(way, c).wait_recv()
                convs = []
                for g, taps in enumerate((gate_taps, up_taps)):
                    here = (part_own[way, c, g] + part_recv[way, c, g].astype(f32)).astype(bf16)
                    here = here.astype(f32)
                    earlier, later = pltpu.roll(here, 1, 0), pltpu.roll(here, reach - 1, 0)
                    if way == 0:
                        earlier = jnp.where(row_at == 0, 0.0, earlier)
                    else:
                        later = jnp.where(row_at == reach - 1, 0.0, later)
                    weight = taps[:, cols].astype(f32)
                    convs.append(weight[0:1] * earlier + weight[1:2] * here + weight[2:3] * later)
                hidden = ((convs[0] / (1.0 + jnp.exp(-convs[0]))) * convs[1]).astype(bf16)
                at = way * EDGE
                hidden_all[way * half : (way + 1) * half, cols] = hidden[at : at + half]

        ready = min(max(0, turn - SKEW * (last - 1) + 1), len(pieces))
        if ready < len(pieces):
            ready = min(ready, 2 * max(0, turn + 1 + HEADSTART - len(pieces)))
        while issued < ready:
            for way in range(2):
                start_hidden(way, issued)
            issued += 1

    for turn in range(len(pieces) + SKEW * (last - 1)):
        for way in range(2):
            for hop in range(1, spans):
                c = turn - SKEW * (hop - 1)
                if 0 <= c < len(pieces):

                    @pl.when(last - hops[way] == hop)
                    def _():
                        hidden_copy(way, c).wait_recv()
                        if hop < last:
                            hidden_copy(way, c).start()

    loads[6].wait()
    near_first = list(range(spans))
    fans = {}
    for d in near_first:
        source = lax.rem(me + spans - d, spans)
        tp_send[d] = lax.dot_general(
            hidden_all[span_rows(source), :],
            down_w[...],
            (((1,), (1,)), ((), ())),
            preferred_element_type=f32,
        ).astype(bf16)
        for b in range(1, shares):
            fans[d, b] = send(
                tp_send.at[d, share_rows(share_at(b))],
                tp_recv.at[d, b],
                tp_sem.at[d, b],
                me,
                share_at(b),
            )
    arrivals = []
    for d in near_first:
        source = lax.rem(me + spans - d, spans)
        summed = tp_send[d, share_rows(lane), :].astype(f32)
        for b in range(1, shares):
            fans[d, b].wait_recv()
            summed = summed + tp_recv[d, b].astype(f32)
        row_send[d] = summed.astype(bf16)
        if d:
            arrivals.append(send(row_send.at[d], row_recv.at[me], row_sem.at[d], source, lane))
        else:
            row_recv[me] = row_send[0]
    for copy in arrivals:
        copy.wait_recv()
    for j in range(spans):
        cols = slice(j * part_cols, (j + 1) * part_cols)
        result[:, cols] = (middle_ref[:, cols].astype(f32) + row_recv[j].astype(f32)).astype(bf16)
    for copy in sends:
        copy.wait_send()
    for c in range(len(pieces)):
        for way in range(2):

            middle_span = (me != owners[way]) & (me != origins[way])
            unwaited = c + FLIGHT >= len(pieces)

            @pl.when(middle_span | ((me == origins[way]) & unwaited))
            def _():
                part_copy(way, c).wait_send()

            @pl.when(middle_span | ((me == owners[way]) & unwaited))
            def _():
                hidden_copy(way, c).wait_send()


def fused_block(
    query_rows,
    key_rows,
    value_rows,
    gate_rows,
    log_decay,
    head_gain,
    out_weight,
    residual,
    norm_gain,
    gate_weight,
    up_weight,
    down_weight,
    gate_taps,
    up_taps,
):
    spans, shares = (lax.axis_size("sp"), lax.axis_size("tp"))
    rows, width = query_rows.shape
    model = residual.shape[1]
    units = gate_weight.shape[1]
    part_cols, share = (model // spans, rows // shares)
    total = spans * rows
    lanes = units // 128
    count = max(n for n in range(1, PIECES + 1) if lanes % n == 0)
    size = units // count
    pieces = [(c * size, size) for c in range(count)]
    reach = total // 2 + EDGE
    lines = log_decay.shape[0] * log_decay.shape[1]
    rates = log_decay.reshape(lines, rows)
    f32, bf16 = jnp.float32, jnp.bfloat16
    vmem = pl.BlockSpec(memory_space=pltpu.VMEM)
    far = pl.BlockSpec(memory_space=pl.ANY)
    dma = pltpu.SemaphoreType.DMA
    return pl.pallas_call(
        functools.partial(block_kernel, spans, shares, tuple(pieces)),
        out_shape=jax.ShapeDtypeStruct((share, model), bf16),
        in_specs=[vmem] * 10 + [far] * 4,
        out_specs=vmem,
        scratch_shapes=[
            pltpu.VMEM((total, width), bf16),
            pltpu.VMEM((total, width), bf16),
            pltpu.VMEM((spans, lines, rows), f32),
            pltpu.VMEM(out_weight.shape, bf16),
            pltpu.VMEM((2, *gate_weight.shape), bf16),
            pltpu.VMEM(down_weight.shape, bf16),
            pltpu.VMEM((rows, model), bf16),
            pltpu.VMEM((shares, share, model), bf16),
            pltpu.VMEM((share, model), bf16),
            pltpu.VMEM((spans, share, part_cols), bf16),
            pltpu.VMEM((total, part_cols), bf16),
            pltpu.VMEM((2, count, 2, reach, size), bf16),
            pltpu.VMEM((2, count, 2, reach, size), f32),
            pltpu.VMEM((2, count, 2, reach, size), bf16),
            pltpu.VMEM((total, units), bf16),
            pltpu.VMEM((spans, rows, part_cols), bf16),
            pltpu.VMEM((spans, shares, share, part_cols), bf16),
            pltpu.VMEM((spans, share, part_cols), bf16),
            pltpu.VMEM((spans, share, part_cols), bf16),
            dma((7,)),
            dma((spans, 3, 2)),
            dma((shares, 2)),
            dma((spans, 2)),
            dma((spans, shares, 2)),
            dma((2, count, 2)),
            dma((2, count, 2)),
            dma((spans, shares, 2)),
            dma((spans, 2)),
        ],
        compiler_params=pltpu.CompilerParams(collective_id=0, has_side_effects=True),
    )(
        query_rows,
        key_rows,
        value_rows,
        gate_rows,
        rates,
        head_gain,
        residual,
        norm_gain.reshape(1, model),
        gate_taps,
        up_taps,
        out_weight,
        gate_weight,
        up_weight,
        down_weight,
    )


def either(*args):
    span_tokens = args[0].shape[0] * lax.axis_size("sp")
    model_width = args[7].shape[1]
    if span_tokens < model_width:
        return fused_block(*args)
    return shards(*args)


def solution(mesh):
    in_specs = (
        P(("grp", "sp"), "tp"),
        P(("grp", "sp"), "tp"),
        P(("grp", "sp"), "tp"),
        P(("grp", "sp"), "tp"),
        P(None, "tp", ("grp", "sp")),
        P(None, "tp"),
        P("tp", None),
        P(("grp", "sp"), None),
        P(),
        P("sp", "tp"),
        P("sp", "tp"),
        P("sp", "tp"),
        P(None, "tp"),
        P(None, "tp"),
    )
    out_specs = P(("grp", "sp", "tp"), None)
    return jax.shard_map(either, mesh=mesh, in_specs=in_specs, out_specs=out_specs, check_vma=False)
```

```python
import functools
import math

import jax
import jax.numpy as jnp
from jax import lax
from jax.experimental import pallas as pl
from jax.experimental.pallas import tpu as pltpu
from jax.sharding import PartitionSpec as P

HEAD = 128
PIECES = 12
EDGE = 16
FLIGHT = 2
HEADSTART = 2
SKEW = 2


FULL_PRECISION = lax.Precision.HIGHEST
GROUP_EPS = 1e-05
NORM_EPS = 1e-06


def prefix(value, axis, join, neutral, backward):
    count, mine = (lax.axis_size(axis), lax.axis_index(axis))
    pieces = jax.tree.map(lambda part: lax.all_gather(part, axis), value)
    if backward:
        pieces = jax.tree.map(lambda part: part[::-1], pieces)
        mine = count - 1 - mine
    running = jax.tree.map(
        lambda part, zero: jnp.full_like(part, 0) + jnp.asarray(zero, part.dtype), value, neutral
    )

    def lap(position, running):
        longer = join(running, jax.tree.map(lambda part: part[position], pieces))
        return jax.tree.map(lambda new, old: jnp.where(position < mine, new, old), longer, running)

    return lax.fori_loop(0, count - 1, lap, running)


def padded_2(shard, sides, width):
    for axis, dim in sides:
        size, length = (lax.axis_size(axis), shard.shape[dim])
        up = [(i, (i + 1) % size) for i in range(size - 1)]
        down = [(j, i) for i, j in up]
        last = lax.slice_in_dim(shard, length - width, length, axis=dim)
        initial = lax.slice_in_dim(shard, 0, width, axis=dim)
        before = lax.ppermute(last, axis, up)
        after = lax.ppermute(initial, axis, down)
        shard = jnp.concatenate([before, shard, after], axis=dim)
    return shard


def state_combine(earlier, later):
    return (earlier[0] * later[0], earlier[1] * later[0][:, None, None] + later[1])


def group_norm(values):
    length, head_count, head_width = values.shape
    centre = values - jnp.mean(values, axis=2, keepdims=True)
    spread = jnp.mean(centre * centre, axis=2, keepdims=True)
    return (centre * lax.rsqrt(spread + GROUP_EPS)).reshape(length, head_count * head_width)


def rms_scale(middle, gain):
    values = middle.astype(jnp.float32)
    multiplier = lax.rsqrt(jnp.mean(values * values, axis=1, keepdims=True) + NORM_EPS)
    return (values * multiplier * gain.astype(jnp.float32)).astype(jnp.bfloat16)


def local_retention(query_all, key_all, value_all, log_rates):
    length, head_count, head_width = query_all.shape
    block_len = math.gcd(length, 512)
    block_count = length // block_len
    cumul = jnp.cumsum(log_rates, axis=1).T
    query_block = query_all.reshape(block_count, block_len, head_count, head_width)
    key_block = key_all.reshape(block_count, block_len, head_count, head_width)
    value_block = value_all.reshape(block_count, block_len, head_count, head_width)
    cumul_block = cumul.reshape(block_count, block_len, head_count)
    before = jnp.concatenate(
        [jnp.zeros((1, head_count), jnp.float32), cumul_block[:-1, -1]], axis=0
    )
    local_cumul = cumul_block - before[:, None, :]
    gap_logs = local_cumul[:, :, None, :] - local_cumul[:, None, :, :]
    lower_mask = (jnp.arange(block_len)[:, None] >= jnp.arange(block_len)[None, :])[
        None, :, :, None
    ]
    decay_mask = jnp.where(lower_mask, jnp.exp(jnp.minimum(gap_logs, 0.0)), 0.0)
    scores = (
        jnp.einsum("bthd,bshd->btsh", query_block, key_block, precision=FULL_PRECISION) * decay_mask
    )
    inner_part = jnp.einsum("btsh,bshe->bthe", scores, value_block, precision=FULL_PRECISION)
    to_end = jnp.exp(local_cumul[:, -1:, :] - local_cumul)
    block_states = jnp.einsum(
        "bshd,bshe->bhde", key_block * to_end[..., None], value_block, precision=FULL_PRECISION
    )
    block_decay = jnp.exp(local_cumul[:, -1, :])

    def carry_step(carry_state, inputs):
        return (carry_state * inputs[0][:, None, None] + inputs[1], carry_state)

    zero_state = jnp.zeros((head_count, head_width, head_width), jnp.float32)
    end_state, entering = lax.scan(carry_step, zero_state, (block_decay, block_states))
    carried = jnp.einsum(
        "bthd,bhde->bthe",
        query_block * jnp.exp(local_cumul)[..., None],
        entering,
        precision=FULL_PRECISION,
    )
    output = (inner_part + carried).reshape(length, head_count, head_width)
    return (output, end_state, cumul, jnp.exp(cumul[-1]))


def with_incoming(output, query_all, cumul, incoming):
    return output + jnp.einsum(
        "thd,hde->the", query_all * jnp.exp(cumul)[:, :, None], incoming, precision=FULL_PRECISION
    )


def shards(
    query_rows,
    key_rows,
    value_rows,
    gate_rows,
    log_decay,
    head_gain,
    out_weight,
    residual,
    norm_gain,
    gate_weight,
    up_weight,
    down_weight,
    gate_taps,
    up_taps,
):
    pair_local = jnp.concatenate([gate_weight, up_weight], axis=1)
    row_count = query_rows.shape[0]
    head_count = query_rows.shape[1] // HEAD
    key_scale = HEAD ** (-0.5)
    query_all = query_rows.astype(jnp.float32).reshape(row_count, head_count, HEAD)
    key_all = key_rows.astype(jnp.float32).reshape(row_count, head_count, HEAD) * key_scale
    value_all = value_rows.astype(jnp.float32).reshape(row_count, head_count, HEAD)
    identity = (
        jnp.ones((head_count,), jnp.float32),
        jnp.zeros((head_count, HEAD, HEAD), jnp.float32),
    )
    ahead_local, ahead_state, ahead_cumul, ahead_decay = local_retention(
        query_all, key_all, value_all, log_decay[0]
    )
    query_back = query_all[::-1]
    behind_local, behind_state, behind_cumul, behind_decay = local_retention(
        query_back, key_all[::-1], value_all[::-1], log_decay[1][:, ::-1]
    )
    ahead_in = prefix((ahead_decay, ahead_state), "sp", state_combine, identity, False)[1]
    behind_in = prefix((behind_decay, behind_state), "sp", state_combine, identity, True)[1]
    ahead_out = with_incoming(ahead_local, query_all, ahead_cumul, ahead_in)
    behind_out = with_incoming(behind_local, query_back, behind_cumul, behind_in)[::-1]
    combined = group_norm(ahead_out) * head_gain[0] + group_norm(behind_out) * head_gain[1]
    mixed_heads = (jax.nn.silu(gate_rows.astype(jnp.float32)) * combined).astype(jnp.bfloat16)
    gathered = (
        lax.all_gather(pair_local, "sp", axis=0, tiled=True),
        lax.all_gather(down_weight, "sp", axis=0, tiled=True),
    )
    pair_full, down_full = gathered
    share_rows = row_count // lax.axis_size("tp")
    own_start = lax.axis_index("tp") * share_rows
    picked = mixed_heads
    attended = lax.psum_scatter(
        jnp.dot(picked, out_weight, preferred_element_type=jnp.float32).astype(jnp.bfloat16),
        "tp",
        scatter_dimension=0,
        tiled=True,
    ).astype(jnp.float32)
    residual_own = lax.dynamic_slice_in_dim(residual, own_start, share_rows, 0)
    middle_own = lax.optimization_barrier(
        (residual_own.astype(jnp.float32) + attended).astype(jnp.bfloat16)
    )
    normed = rms_scale(middle_own, norm_gain)
    pre_both = jnp.dot(
        lax.all_gather(normed, "tp", axis=0, tiled=True),
        pair_full,
        preferred_element_type=jnp.float32,
    ).astype(jnp.bfloat16)
    padded = padded_2(pre_both, (("sp", 0),), 1)
    half_width = gate_taps.shape[1]
    tap_table = jnp.concatenate([gate_taps, up_taps], axis=1).astype(jnp.float32)
    conv_out = (
        tap_table[0] * padded[:-2].astype(jnp.float32)
        + tap_table[1] * padded[1:-1].astype(jnp.float32)
        + tap_table[2] * padded[2:].astype(jnp.float32)
    )
    hidden = (jax.nn.silu(conv_out[:, :half_width]) * conv_out[:, half_width:]).astype(jnp.bfloat16)
    picked = hidden
    ff_out = lax.psum_scatter(
        lax.dot_general(
            picked, down_full, (((1,), (1,)), ((), ())), preferred_element_type=jnp.float32
        ).astype(jnp.bfloat16),
        "tp",
        scatter_dimension=0,
        tiled=True,
    ).astype(jnp.float32)
    return (middle_own.astype(jnp.float32) + ff_out).astype(jnp.bfloat16)


def block_kernel(
    spans,
    shares,
    pieces,
    query,
    key,
    value,
    gate,
    rates,
    gains,
    residual,
    norm_gain,
    gate_taps,
    up_taps,
    out_hbm,
    gate_hbm,
    up_hbm,
    down_hbm,
    result,
    keys,
    values,
    rate_all,
    out_w,
    pair_w,
    down_w,
    att_send,
    att_recv,
    middle_ref,
    norm_send,
    norm_all,
    part_send,
    part_own,
    part_recv,
    hidden_all,
    tp_send,
    tp_recv,
    row_send,
    row_recv,
    local_sem,
    kv_sem,
    att_sem,
    norm_sem,
    fan_sem,
    part_sem,
    hid_sem,
    tp_sem,
    row_sem,
):
    me, lane = lax.axis_index("sp"), lax.axis_index("tp")
    rows, width = query.shape
    heads = width // HEAD
    share = rows // shares
    model = residual.shape[1]
    part_cols = model // spans
    f32, bf16 = jnp.float32, jnp.bfloat16
    sends = []

    def send(src, dst, sems, sp, tp):
        copy = pltpu.make_async_remote_copy(
            src_ref=src,
            dst_ref=dst,
            send_sem=sems.at[0],
            recv_sem=sems.at[1],
            device_id={"sp": sp, "tp": tp},
            device_id_type=pl.DeviceIdType.MESH,
        )
        copy.start()
        sends.append(copy)
        return copy

    def span_at(step):
        return lax.rem(me + step, spans)

    def share_at(step):
        return lax.rem(lane + step, shares)

    def span_rows(index):
        return pl.ds(pl.multiple_of(index * rows, rows), rows)

    loads = [
        pltpu.make_async_copy(src, dst, local_sem.at[i])
        for i, (src, dst) in enumerate(
            (
                (key, keys.at[span_rows(me)]),
                (value, values.at[span_rows(me)]),
                (rates, rate_all.at[me]),
                (out_hbm, out_w),
                (gate_hbm, pair_w.at[0]),
                (up_hbm, pair_w.at[1]),
                (down_hbm, down_w),
            )
        )
    ]
    for load in loads:
        load.start()
    barrier = pltpu.get_barrier_semaphore()
    for a in range(spans):
        for b in range(shares):
            if a or b:
                pl.semaphore_signal(
                    barrier,
                    inc=1,
                    device_id={"sp": span_at(a), "tp": share_at(b)},
                    device_id_type=pl.DeviceIdType.MESH,
                )
    pl.semaphore_wait(barrier, spans * shares - 1)

    arrivals = []
    for d in range(1, spans):
        to = span_at(d)
        arrivals += [
            send(rates, rate_all.at[me], kv_sem.at[d, 0], to, lane),
            send(key, keys.at[span_rows(me)], kv_sem.at[d, 1], to, lane),
            send(value, values.at[span_rows(me)], kv_sem.at[d, 2], to, lane),
        ]
    for load in loads[:3]:
        load.wait()
    for copy in arrivals:
        copy.wait_recv()

    low = lax.broadcasted_iota(jnp.int32, (rows, rows), 0)
    high = lax.broadcasted_iota(jnp.int32, (rows, rows), 1)
    upto = (low <= high).astype(f32)
    since = (low >= high).astype(f32)
    lines = rates.shape[0]
    offset = jnp.zeros((lines, 1), f32)
    offset_own = jnp.zeros((lines, 1), f32)
    cumuls = []
    for j in range(spans):
        offset_own = jnp.where(j == me, offset, offset_own)
        inside = jnp.dot(rate_all[j], upto, precision=FULL_PRECISION, preferred_element_type=f32)
        cumuls.append(inside + offset)
        offset = offset + inside[:, rows - 1 :]
    cumul = jnp.concatenate(cumuls, axis=1)
    every_rate = jnp.concatenate([rate_all[j] for j in range(spans)], axis=1)
    own_rate = rates[...]
    own_cumul = lax.dot_general(
        since,
        own_rate,
        (((1,), (1,)), ((), ())),
        precision=FULL_PRECISION,
        preferred_element_type=f32,
    )
    own_before = lax.dot_general(
        (low > high).astype(f32),
        own_rate,
        (((1,), (1,)), ((), ())),
        precision=FULL_PRECISION,
        preferred_element_type=f32,
    )
    total = spans * rows
    mine_at = lax.broadcasted_iota(jnp.int32, (rows, total), 0) + me * rows
    other_at = lax.broadcasted_iota(jnp.int32, (rows, total), 1)
    mixed = []
    for head in range(heads):
        cols = slice(head * HEAD, (head + 1) * HEAD)
        scores = lax.dot_general(
            query[:, cols],
            keys[:, cols],
            (((1,), (1,)), ((), ())),
            preferred_element_type=f32,
        ) * (HEAD ** (-0.5))
        back = heads + head
        ahead_gap = (own_cumul[:, head : head + 1] + offset_own[head : head + 1]) - cumul[
            head : head + 1
        ]
        behind_gap = (cumul[back : back + 1] - every_rate[back : back + 1]) - (
            own_before[:, back : back + 1] + offset_own[back : back + 1]
        )
        sides = []
        for gap, keep, row in (
            (ahead_gap, mine_at >= other_at, 0),
            (behind_gap, mine_at <= other_at, 1),
        ):
            weighted = jnp.where(keep, jnp.exp(jnp.minimum(gap, 0.0)), 0.0) * scores
            top = weighted.astype(bf16)
            rest = (weighted - top.astype(f32)).astype(bf16)
            held = values[:, cols]
            out = jnp.dot(top, held, preferred_element_type=f32) + jnp.dot(
                rest, held, preferred_element_type=f32
            )
            centre = out - jnp.mean(out, axis=1, keepdims=True)
            spread = jnp.mean(centre * centre, axis=1, keepdims=True)
            sides.append(centre * lax.rsqrt(spread + GROUP_EPS) * gains[row : row + 1, cols])
        level = gate[:, cols].astype(f32)
        mixed.append(((level / (1.0 + jnp.exp(-level))) * (sides[0] + sides[1])).astype(bf16))
    mixed = jnp.concatenate(mixed, axis=1)

    loads[3].wait()
    step_cols = math.gcd(model, 512)
    for at in range(0, model, step_cols):
        att_send[:, at : at + step_cols] = jnp.dot(
            mixed, out_w[:, at : at + step_cols], preferred_element_type=f32
        ).astype(bf16)

    def share_rows(index):
        return pl.ds(pl.multiple_of(index * share, share), share)

    arrivals = [
        send(
            att_send.at[share_rows(share_at(d))],
            att_recv.at[d],
            att_sem.at[d],
            me,
            share_at(d),
        )
        for d in range(1, shares)
    ]
    attended = att_send[share_rows(lane), :].astype(f32)
    for d, copy in enumerate(arrivals, 1):
        copy.wait_recv()
        attended = attended + att_recv[d].astype(f32)
    middle = (residual[share_rows(lane), :].astype(f32) + attended).astype(bf16)
    middle_ref[...] = middle
    middle = middle.astype(f32)
    factor = lax.rsqrt(jnp.mean(middle * middle, axis=1, keepdims=True) + NORM_EPS)
    normed = (middle * factor * norm_gain[...].astype(f32)).astype(bf16)
    for j in range(spans):
        norm_send[j] = normed[:, j * part_cols : (j + 1) * part_cols]

    def token_rows(span, tp):
        return pl.ds(pl.multiple_of(span * rows + tp * share, share), share)

    arrivals = [
        send(
            norm_send.at[span_at(d)],
            norm_all.at[token_rows(me, lane)],
            norm_sem.at[d],
            span_at(d),
            lane,
        )
        for d in range(1, spans)
    ]
    norm_all[token_rows(me, lane), :] = norm_send[me]
    fans = {}
    for d in (0, *range(1, spans)):
        source = lax.rem(me + spans - d, spans)
        if d:
            arrivals[d - 1].wait_recv()
        block = norm_send.at[me] if d == 0 else norm_all.at[token_rows(source, lane)]
        for b in range(1, shares):
            fans[d, b] = send(
                block, norm_all.at[token_rows(source, lane)], fan_sem.at[d, b], me, share_at(b)
            )
    for copy in fans.values():
        copy.wait_recv()

    loads[4].wait()
    loads[5].wait()
    last = spans - 1
    half = spans * rows // 2
    reach = half + EDGE
    size = pieces[0][1]
    origins, owners = (last, 0), (0, last)

    def part_copy(way, c):
        return pltpu.make_async_remote_copy(
            src_ref=part_send.at[way, c],
            dst_ref=part_recv.at[way, c],
            send_sem=part_sem.at[way, c, 0],
            recv_sem=part_sem.at[way, c, 1],
            device_id={"sp": span_at(spans - 1 if way == 0 else 1), "tp": lane},
            device_id_type=pl.DeviceIdType.MESH,
        )

    def hidden_copy(way, c):
        block = hidden_all.at[pl.ds(way * half, half), pl.ds(pieces[c][0], size)]
        return pltpu.make_async_remote_copy(
            src_ref=block,
            dst_ref=block,
            send_sem=hid_sem.at[way, c, 0],
            recv_sem=hid_sem.at[way, c, 1],
            device_id={"sp": span_at(1 if way == 0 else spans - 1), "tp": lane},
            device_id_type=pl.DeviceIdType.MESH,
        )

    def start_part(way, c):
        @pl.when(me == origins[way])
        def _():
            if c >= FLIGHT:
                part_copy(way, c - FLIGHT).wait_send()
            part_copy(way, c).start()

    def start_hidden(way, c):
        @pl.when(me == owners[way])
        def _():
            if c >= FLIGHT:
                hidden_copy(way, c - FLIGHT).wait_send()
            hidden_copy(way, c).start()

    def project(c):
        cols = slice(pieces[c][0], pieces[c][0] + size)
        for way in range(2):
            at = way * (half - EDGE)
            block = norm_all[at : at + reach, :]
            products = [
                jnp.dot(block, pair_w[g, :, cols], preferred_element_type=f32) for g in range(2)
            ]

            @pl.when(me == origins[way])
            def _():
                for g in range(2):
                    part_send[way, c, g] = products[g].astype(bf16)

            start_part(way, c)

            @pl.when(me != origins[way])
            def _():
                for g in range(2):
                    part_own[way, c, g] = products[g]

    for c in range(min(HEADSTART, len(pieces))):
        project(c)

    row_at = lax.broadcasted_iota(jnp.int32, (reach, 1), 0)
    issued = 0
    hops = (last - me, me)
    for turn in range(len(pieces) + SKEW * (last - 1)):
        if turn + HEADSTART < len(pieces):
            project(turn + HEADSTART)
        for way in range(2):
            for hop in range(1, last):
                c = turn - SKEW * (hop - 1)
                if 0 <= c < len(pieces):

                    @pl.when(hops[way] == hop)
                    def _():
                        part_copy(way, c).wait_recv()
                        for g in range(2):
                            part_send[way, c, g] = (
                                part_own[way, c, g] + part_recv[way, c, g].astype(f32)
                            ).astype(bf16)
                        part_copy(way, c).start()

            c = turn - SKEW * (last - 1)
            if c < 0:
                continue
            cols = slice(pieces[c][0], pieces[c][0] + size)

            @pl.when(me == owners[way])
            def _():
                part_copy(way, c).wait_recv()
                convs = []
                for g, taps in enumerate((gate_taps, up_taps)):
                    here = (part_own[way, c, g] + part_recv[way, c, g].astype(f32)).astype(bf16)
                    here = here.astype(f32)
                    earlier, later = pltpu.roll(here, 1, 0), pltpu.roll(here, reach - 1, 0)
                    if way == 0:
                        earlier = jnp.where(row_at == 0, 0.0, earlier)
                    else:
                        later = jnp.where(row_at == reach - 1, 0.0, later)
                    weight = taps[:, cols].astype(f32)
                    convs.append(weight[0:1] * earlier + weight[1:2] * here + weight[2:3] * later)
                hidden = ((convs[0] / (1.0 + jnp.exp(-convs[0]))) * convs[1]).astype(bf16)
                at = way * EDGE
                hidden_all[way * half : (way + 1) * half, cols] = hidden[at : at + half]

        ready = min(max(0, turn - SKEW * (last - 1) + 1), len(pieces))
        if ready < len(pieces):
            ready = min(ready, 2 * max(0, turn + 1 + HEADSTART - len(pieces)))
        while issued < ready:
            for way in range(2):
                start_hidden(way, issued)
            issued += 1

    for turn in range(len(pieces) + SKEW * (last - 1)):
        for way in range(2):
            for hop in range(1, spans):
                c = turn - SKEW * (hop - 1)
                if 0 <= c < len(pieces):

                    @pl.when(last - hops[way] == hop)
                    def _():
                        hidden_copy(way, c).wait_recv()
                        if hop < last:
                            hidden_copy(way, c).start()

    loads[6].wait()
    near_first = list(range(spans))
    fans = {}
    for d in near_first:
        source = lax.rem(me + spans - d, spans)
        tp_send[d] = lax.dot_general(
            hidden_all[span_rows(source), :],
            down_w[...],
            (((1,), (1,)), ((), ())),
            preferred_element_type=f32,
        ).astype(bf16)
        for b in range(1, shares):
            fans[d, b] = send(
                tp_send.at[d, share_rows(share_at(b))],
                tp_recv.at[d, b],
                tp_sem.at[d, b],
                me,
                share_at(b),
            )
    arrivals = []
    for d in near_first:
        source = lax.rem(me + spans - d, spans)
        summed = tp_send[d, share_rows(lane), :].astype(f32)
        for b in range(1, shares):
            fans[d, b].wait_recv()
            summed = summed + tp_recv[d, b].astype(f32)
        row_send[d] = summed.astype(bf16)
        if d:
            arrivals.append(send(row_send.at[d], row_recv.at[me], row_sem.at[d], source, lane))
        else:
            row_recv[me] = row_send[0]
    for copy in arrivals:
        copy.wait_recv()
    for j in range(spans):
        cols = slice(j * part_cols, (j + 1) * part_cols)
        result[:, cols] = (middle_ref[:, cols].astype(f32) + row_recv[j].astype(f32)).astype(bf16)
    for copy in sends:
        copy.wait_send()
    for c in range(len(pieces)):
        for way in range(2):

            middle_span = (me != owners[way]) & (me != origins[way])
            unwaited = c + FLIGHT >= len(pieces)

            @pl.when(middle_span | ((me == origins[way]) & unwaited))
            def _():
                part_copy(way, c).wait_send()

            @pl.when(middle_span | ((me == owners[way]) & unwaited))
            def _():
                hidden_copy(way, c).wait_send()


def fused_block(
    query_rows,
    key_rows,
    value_rows,
    gate_rows,
    log_decay,
    head_gain,
    out_weight,
    residual,
    norm_gain,
    gate_weight,
    up_weight,
    down_weight,
    gate_taps,
    up_taps,
):
    spans, shares = (lax.axis_size("sp"), lax.axis_size("tp"))
    rows, width = query_rows.shape
    model = residual.shape[1]
    units = gate_weight.shape[1]
    part_cols, share = (model // spans, rows // shares)
    total = spans * rows
    lanes = units // 128
    count = max(n for n in range(1, PIECES + 1) if lanes % n == 0)
    size = units // count
    pieces = [(c * size, size) for c in range(count)]
    reach = total // 2 + EDGE
    lines = log_decay.shape[0] * log_decay.shape[1]
    rates = log_decay.reshape(lines, rows)
    f32, bf16 = jnp.float32, jnp.bfloat16
    vmem = pl.BlockSpec(memory_space=pltpu.VMEM)
    far = pl.BlockSpec(memory_space=pl.ANY)
    dma = pltpu.SemaphoreType.DMA
    return pl.pallas_call(
        functools.partial(block_kernel, spans, shares, tuple(pieces)),
        out_shape=jax.ShapeDtypeStruct((share, model), bf16),
        in_specs=[vmem] * 10 + [far] * 4,
        out_specs=vmem,
        scratch_shapes=[
            pltpu.VMEM((total, width), bf16),
            pltpu.VMEM((total, width), bf16),
            pltpu.VMEM((spans, lines, rows), f32),
            pltpu.VMEM(out_weight.shape, bf16),
            pltpu.VMEM((2, *gate_weight.shape), bf16),
            pltpu.VMEM(down_weight.shape, bf16),
            pltpu.VMEM((rows, model), bf16),
            pltpu.VMEM((shares, share, model), bf16),
            pltpu.VMEM((share, model), bf16),
            pltpu.VMEM((spans, share, part_cols), bf16),
            pltpu.VMEM((total, part_cols), bf16),
            pltpu.VMEM((2, count, 2, reach, size), bf16),
            pltpu.VMEM((2, count, 2, reach, size), f32),
            pltpu.VMEM((2, count, 2, reach, size), bf16),
            pltpu.VMEM((total, units), bf16),
            pltpu.VMEM((spans, rows, part_cols), bf16),
            pltpu.VMEM((spans, shares, share, part_cols), bf16),
            pltpu.VMEM((spans, share, part_cols), bf16),
            pltpu.VMEM((spans, share, part_cols), bf16),
            dma((7,)),
            dma((spans, 3, 2)),
            dma((shares, 2)),
            dma((spans, 2)),
            dma((spans, shares, 2)),
            dma((2, count, 2)),
            dma((2, count, 2)),
            dma((spans, shares, 2)),
            dma((spans, 2)),
        ],
        compiler_params=pltpu.CompilerParams(collective_id=0, has_side_effects=True),
    )(
        query_rows,
        key_rows,
        value_rows,
        gate_rows,
        rates,
        head_gain,
        residual,
        norm_gain.reshape(1, model),
        gate_taps,
        up_taps,
        out_weight,
        gate_weight,
        up_weight,
        down_weight,
    )


def either(*args):
    span_tokens = args[0].shape[0] * lax.axis_size("sp")
    model_width = args[7].shape[1]
    if span_tokens < model_width:
        return fused_block(*args)
    return shards(*args)


def solution(mesh):
    in_specs = (
        P(("grp", "sp"), "tp"),
        P(("grp", "sp"), "tp"),
        P(("grp", "sp"), "tp"),
        P(("grp", "sp"), "tp"),
        P(None, "tp", ("grp", "sp")),
        P(None, "tp"),
        P("tp", None),
        P(("grp", "sp"), None),
        P(),
        P("sp", "tp"),
        P("sp", "tp"),
        P("sp", "tp"),
        P(None, "tp"),
        P(None, "tp"),
    )
    out_specs = P(("grp", "sp", "tp"), None)
    return jax.shard_map(either, mesh=mesh, in_specs=in_specs, out_specs=out_specs, check_vma=False)
```
